32 devices in a mesh: grp: 2 (over y), sp: 4 (over z), tp: 4 (over x, core).
Axes of the slice: x: 2, y: 2, z: 4, core: 2. Of those that a mesh axis runs over, the one named last changes fastest.
Arguments:
- queries: bfloat16 [4096, 1024], P(('grp', 'sp'), 'tp'), parts along dimension 0, may hold values from -5 to 9
- keys: bfloat16 [4096, 1024], P(('grp', 'sp'), 'tp'), parts along dimension 0, may hold values from -12 to 5
- values: bfloat16 [4096, 1024], P(('grp', 'sp'), 'tp'), parts along dimension 0, may hold values from -5 to 5
- residual: bfloat16 [4096, 2048], P(('grp', 'sp')), parts along dimension 0, may hold values from -6 to 6
- out_weight: bfloat16 [1024, 2048], P('tp'), may hold values from -0.1875 to 0.1875
- post_gain: float32 [2048], replicated, may hold values from 0.1 to 1.9
- gate_weight: bfloat16 [2048, 5120], P('sp', 'tp'), may hold values from -0.125 to 0.125
- up_weight: bfloat16 [2048, 5120], P('sp', 'tp'), may hold values from -0.125 to 0.125
- down_weight: bfloat16 [5120, 2048], P('tp', 'sp'), may hold values from -0.078125 to 0.078125
- ffn_pre_gain: float32 [2048], replicated, may hold values from 0.1 to 1.9
- ffn_post_gain: float32 [2048], replicated, may hold values from 0.1 to 1.9
Outputs:
- layer_out: bfloat16 [4096, 2048], P(('grp', 'sp', 'tp')), parts along dimension 0
The draws below stay inside these ranges and needn't reach their ends.
There are 2 independent parts, one for each index of `grp`. The reference program is written for one: setup_inputs(seed, part) draws one part's arguments, and reference() takes and returns one part's arrays. A program takes and returns all parts, laid end to end along the dimension named above; an argument that names none is the same for every part. Nothing has to cross between parts.
All inputs are finite; a program needn't handle non-finite values.
Results may differ from the reference program's by a relative error of at most 0.014.
Values may be sent and summed in bfloat16 or wider, within the bound.
A program may use at most 64 MiB of HBM per device.

```python
import math
import jax
import jax.numpy as jnp
from jax import lax

D = 2048
HEAD_TOTAL = 16
HEAD_DIM = 64
FF = 5120
TOK_DEV = 512
TOKEN_TOTAL = 2048
N_TP = 4


def draw_queries(key, part):
    noise_random_key, lead_key = jax.random.split(key)
    noise = jnp.clip(jax.random.normal(noise_random_key, (TOKEN_TOTAL, HEAD_TOTAL, HEAD_DIM), jnp.float32), -5.0, 5.0)
    leader_value = jax.random.uniform(lead_key, (TOKEN_TOTAL, HEAD_TOTAL), jnp.float32, 0.875, 1.125) * math.sqrt(HEAD_DIM)
    lead_mask = jnp.arange(HEAD_DIM) == 0
    drawn = jnp.where(lead_mask[None, None, :], leader_value[:, :, None], noise)
    return drawn.reshape(TOKEN_TOTAL, HEAD_TOTAL * HEAD_DIM).astype(jnp.bfloat16)


def draw_keys(key, part):
    split_keys = jax.random.split(key, 7)
    noise_random_key = split_keys[0]
    velocity_random_key = split_keys[1]
    block_random_key = split_keys[2]
    spike_random_key = split_keys[3]
    position_random_key = split_keys[4]
    middle_pick_key = split_keys[5]
    middle_value_key = split_keys[6]
    noise = jnp.clip(jax.random.normal(noise_random_key, (TOKEN_TOTAL, HEAD_TOTAL, HEAD_DIM), jnp.float32), -5.0, 5.0)
    fast_head = jax.random.uniform(velocity_random_key, (HEAD_TOTAL,), jnp.float32) < 0.5
    chain_rate = math.log(TOKEN_TOTAL) + 1.0
    head_rate = jnp.where(fast_head, 3.5, chain_rate)
    blocks = TOKEN_TOTAL // TOK_DEV
    block_shift = jax.random.uniform(block_random_key, (blocks,), jnp.float32, -0.92, 0.92)
    shift_rows = jnp.repeat(block_shift, TOK_DEV)
    leader_value = shift_rows[:, None] - head_rate[None, :]
    middle_picks = jax.random.randint(middle_pick_key, (blocks, 2, HEAD_TOTAL), 0, TOK_DEV)
    middle_rows = jnp.repeat(middle_picks, TOK_DEV, axis=0)
    row_in_block = jnp.arange(TOKEN_TOTAL) % TOK_DEV
    middle_mask = jnp.any(row_in_block[:, None, None] == middle_rows, axis=1)
    middle_mask = jnp.logical_and(middle_mask, jnp.logical_not(fast_head)[None, :])
    middle_value = jax.random.uniform(middle_value_key, (TOKEN_TOTAL, HEAD_TOTAL), jnp.float32, -4.5, -3.0)
    leader_value = jnp.where(middle_mask, middle_value, leader_value)
    spike_row_indices = jax.random.randint(position_random_key, (4,), 0, TOKEN_TOTAL)
    spike_present = jnp.any(jnp.arange(TOKEN_TOTAL)[:, None] == spike_row_indices[None, :], axis=1)
    spike_leader = -jax.random.uniform(spike_random_key, (TOKEN_TOTAL, HEAD_TOTAL), jnp.float32, 0.0, 1.4)
    leader_value = jnp.where(spike_present[:, None], spike_leader, leader_value)
    lead_mask = jnp.arange(HEAD_DIM) == 0
    drawn = jnp.where(lead_mask[None, None, :], leader_value[:, :, None], noise)
    return drawn.reshape(TOKEN_TOTAL, HEAD_TOTAL * HEAD_DIM).astype(jnp.bfloat16)


def block_levels(own_key, extent, pieces, least, top_value):
    level, own = 1.0, jax.random.fold_in(own_key, 6)
    for dim, shards_of in pieces:
        draws = jnp.exp(jax.random.uniform(jax.random.fold_in(own, dim), (shards_of,), jnp.float32, least / len(pieces), top_value / len(pieces)))
        level = level * jnp.repeat(draws, extent[dim] // shards_of).reshape([-1 if axis == dim else 1 for axis in range(len(extent))])
    return level


def gaussian(own_key, extent, deviation, limit, cuts=(), held_as=jnp.bfloat16):
    entries = deviation * jax.random.normal(own_key, extent, jnp.float32)
    if cuts:
        entries = entries * block_levels(own_key, extent, cuts, -0.22, 0.18)
    return jnp.clip(entries, -limit, limit).astype(held_as)


def setup_inputs(seed: int = 0, part: int = 0) -> dict:
    key_of = jax.random.split(jax.random.key(seed), 12)
    own_keys = jax.random.split(jax.random.fold_in(key_of[11], part), 12)
    return {
        "queries": draw_queries(jax.random.fold_in(jax.random.fold_in(key_of[11], part), 71), part),
        "keys": draw_keys(jax.random.fold_in(jax.random.fold_in(key_of[11], part), 71), part),
        "values": gaussian(own_keys[2], (TOKEN_TOTAL, HEAD_TOTAL * HEAD_DIM), 1.0, 5.0, ((0, 4), (1, 4))),
        "residual": gaussian(own_keys[3], (TOKEN_TOTAL, D), 1.0, 6.0, ((0, 4),)),
        "out_weight": gaussian(key_of[4], (HEAD_TOTAL * HEAD_DIM, D), (HEAD_TOTAL * HEAD_DIM) ** -0.5, 0.1875, ((0, 4),)),
        "post_gain": jnp.clip(1.0 + 0.18 * jax.random.normal(key_of[5], (D,), jnp.float32), 0.1, 1.9),
        "gate_weight": gaussian(key_of[6], (D, FF), D ** -0.5, 0.125, ((0, 4), (1, 4))),
        "up_weight": gaussian(key_of[7], (D, FF), D ** -0.5, 0.125, ((0, 4), (1, 4))),
        "down_weight": gaussian(key_of[8], (FF, D), FF ** -0.5, 0.078125, ((0, 4), (1, 4))),
        "ffn_pre_gain": jnp.clip(1.0 + 0.18 * jax.random.normal(key_of[9], (D,), jnp.float32), 0.1, 1.9),
        "ffn_post_gain": jnp.clip(1.0 + 0.18 * jax.random.normal(key_of[10], (D,), jnp.float32), 0.1, 1.9),
    }


norm_eps = 1e-06

def rms_scale(row_block, gain):
    mean_square = lax.optimization_barrier(jnp.mean(row_block * row_block, axis=-1, keepdims=True))
    return row_block * lax.rsqrt(mean_square + norm_eps) * gain

def group_sum(left, right, group_width):
    groups = left.shape[1] // group_width

    def add_group(acc, group_index):
        left_cols = lax.dynamic_slice_in_dim(left, group_index * group_width, group_width, 1)
        right_rows = lax.dynamic_slice_in_dim(right, group_index * group_width, group_width, 0)
        partial_sum = jnp.dot(left_cols, right_rows, preferred_element_type=jnp.float32).astype(jnp.bfloat16)
        partial_sum = lax.optimization_barrier(partial_sum)
        return (acc + partial_sum.astype(jnp.float32), None)
    summed, unused = lax.scan(add_group, jnp.zeros((left.shape[0], right.shape[1]), jnp.float32), jnp.arange(groups, dtype=jnp.int32))
    return summed

def reference(queries, keys, values, residual, out_weight, post_gain, gate_weight, up_weight, down_weight, ffn_pre_gain, ffn_post_gain):
    key_total = queries.shape[0]
    key_span = math.gcd(512, key_total)
    score_scale = 1.0 / math.sqrt(HEAD_DIM)
    positions = jnp.arange(key_total, dtype=jnp.int32)
    q_heads = queries.reshape(key_total, HEAD_TOTAL, HEAD_DIM).transpose(1, 0, 2)
    k_heads = keys.reshape(key_total, HEAD_TOTAL, HEAD_DIM).transpose(1, 0, 2)
    v_heads = values.reshape(key_total, HEAD_TOTAL, HEAD_DIM).transpose(1, 0, 2)

    def stick_head(head_args):
        q_head, k_head, v_head = head_args

        def one_block(block_index):
            row_start = block_index * key_span
            q_rows = lax.dynamic_slice_in_dim(q_head, row_start, key_span, 0)
            scores = jnp.dot(q_rows, k_head.T, preferred_element_type=jnp.float32) * score_scale
            q_pos = row_start + jnp.arange(key_span, dtype=jnp.int32)
            strict = positions[None, :] < q_pos[:, None]
            fall_log = jnp.where(strict, jax.nn.log_sigmoid(-scores), 0.0)
            later_sum = lax.cumsum(fall_log, axis=1, reverse=True) - fall_log
            weights = jnp.where(strict, jnp.exp(jax.nn.log_sigmoid(scores) + later_sum), 0.0)
            return jnp.dot(weights.astype(jnp.bfloat16), v_head, preferred_element_type=jnp.float32)
        blocks_out = lax.map(one_block, jnp.arange(key_total // key_span, dtype=jnp.int32))
        return blocks_out.reshape(key_total, HEAD_DIM)
    heads_out = lax.map(stick_head, (q_heads, k_heads, v_heads))
    attended = heads_out.transpose(1, 0, 2).reshape(key_total, HEAD_TOTAL * HEAD_DIM).astype(jnp.bfloat16)
    mixed_sum = group_sum(attended, out_weight, HEAD_TOTAL // N_TP * HEAD_DIM)
    first_sum = residual.astype(jnp.float32) + rms_scale(mixed_sum, post_gain)
    ffn_in = rms_scale(first_sum, ffn_pre_gain).astype(jnp.bfloat16)
    gate_sum = jnp.dot(ffn_in, gate_weight, preferred_element_type=jnp.float32)
    up_sum = jnp.dot(ffn_in, up_weight, preferred_element_type=jnp.float32)
    hidden = (jax.nn.silu(gate_sum) * up_sum).astype(jnp.bfloat16)
    ffn_out = group_sum(hidden, down_weight, FF // N_TP)
    return (first_sum + 0.5 * rms_scale(ffn_out, ffn_post_gain)).astype(jnp.bfloat16)
```

```python
import functools
import math

import jax
import jax.numpy as jnp
from jax import lax
from jax.experimental import pallas as pl
from jax.experimental.pallas import tpu as pltpu
from jax.sharding import PartitionSpec as P

HEAD_DIM = 64


norm_eps = 1e-06


def rms_scale(row_block, gain):
    mean_square = jnp.mean(row_block * row_block, axis=-1, keepdims=True)
    return row_block * lax.rsqrt(mean_square + norm_eps) * gain


def attention_block(q_ref, k_ref, v_ref, acc_ref, gone_ref, block_index, span, masked):
    rows = q_ref.shape[1]
    key_rows = pl.ds(pl.multiple_of(block_index * span, span), span)
    key_block = k_ref[key_rows, :]
    value_block = v_ref[key_rows, :]
    row_iota = lax.broadcasted_iota(jnp.int32, (span, span), 0)
    col_iota = lax.broadcasted_iota(jnp.int32, (span, span), 1)
    later = jnp.where(row_iota > col_iota, 1.0, 0.0).astype(jnp.bfloat16)
    lane_head = lax.broadcasted_iota(jnp.int32, acc_ref.shape, 1) // HEAD_DIM
    for head in range(q_ref.shape[0]):
        scores = lax.dot_general(
            q_ref[head], key_block, (((1,), (1,)), ((), ())), preferred_element_type=jnp.float32
        )
        soft = jnp.maximum(scores, 0.0) + jnp.log(1.0 + jnp.exp(-jnp.abs(scores)))
        expo = scores - soft
        if masked:
            strict = col_iota < row_iota
            soft = jnp.where(strict, soft, 0.0)
        tail = jnp.dot(soft.astype(jnp.bfloat16), later, preferred_element_type=jnp.float32)
        gone = gone_ref[head]
        wide = jnp.concatenate([gone] * (span // gone.shape[1]), axis=1)
        weights = jnp.exp(expo - (tail + wide))
        if masked:
            weights = jnp.where(strict, weights, 0.0)
        part = jnp.dot(
            weights.astype(jnp.bfloat16), value_block, preferred_element_type=jnp.float32
        )
        acc_ref[...] += jnp.where(lane_head == head, part, 0.0)
        total = tail[:, :1] + soft[:, :1]
        gone_ref[head] = gone + jnp.broadcast_to(total, gone.shape)


def attention_kernel(row_ref, q_ref, k_ref, v_ref, out_ref, acc_ref, gone_ref, *, span):
    diagonal = row_ref[0] // span + pl.program_id(1)
    acc_ref[...] = jnp.zeros_like(acc_ref)
    gone_ref[...] = jnp.zeros_like(gone_ref)
    attention_block(q_ref, k_ref, v_ref, acc_ref, gone_ref, diagonal, span, True)

    def turn(step, carry):
        attention_block(
            q_ref, k_ref, v_ref, acc_ref, gone_ref, diagonal - 1 - step, span, False
        )
        return carry

    lax.fori_loop(0, diagonal, turn, 0)
    out_ref[...] = acc_ref[...].astype(out_ref.dtype)


def stick_attention(queries, keys_values, first_row):
    tok_rows, width = queries.shape
    key_total = keys_values.shape[0]
    span = math.gcd(256, tok_rows)
    lanes = 128
    pack = lanes // HEAD_DIM
    column_groups = width // lanes
    lane_head = (jnp.arange(width) % lanes) // HEAD_DIM
    scaled = queries * jnp.asarray(1.0 / math.sqrt(HEAD_DIM), queries.dtype)
    split_queries = jnp.stack(
        [jnp.where(lane_head[None, :] == head, scaled, jnp.zeros_like(scaled)) for head in range(pack)]
    )
    grid_spec = pltpu.PrefetchScalarGridSpec(
        num_scalar_prefetch=1,
        grid=(column_groups, tok_rows // span),
        in_specs=[
            pl.BlockSpec((pack, span, lanes), lambda p, i, row: (0, i, p)),
            pl.BlockSpec((key_total, lanes), lambda p, i, row: (0, p)),
            pl.BlockSpec((key_total, lanes), lambda p, i, row: (0, column_groups + p)),
        ],
        out_specs=pl.BlockSpec((span, lanes), lambda p, i, row: (i, p)),
        scratch_shapes=[
            pltpu.VMEM((span, lanes), jnp.float32),
            pltpu.VMEM((pack, span, lanes), jnp.float32),
        ],
    )
    return pl.pallas_call(
        functools.partial(attention_kernel, span=span),
        grid_spec=grid_spec,
        out_shape=jax.ShapeDtypeStruct((tok_rows, width), jnp.bfloat16),
        compiler_params=pltpu.CompilerParams(vmem_limit_bytes=40 * 2**20),
        name="stick_attention",
    )(jnp.reshape(first_row, (1,)).astype(jnp.int32), split_queries, keys_values, keys_values)


def half_gather(weight, side):
    half = weight.shape[0] // 2
    mine = lax.dynamic_slice_in_dim(weight, side * half, half, 0)
    mine = lax.all_gather(mine, "sp", axis=0, tiled=True)
    other = lax.ppermute(mine, "grp", [(0, 1), (1, 0)])
    return mine, other


def per_device(
    queries,
    keys,
    values,
    residual,
    out_weight,
    post_gain,
    gate_weight,
    up_weight,
    down_weight,
    ffn_pre_gain,
    ffn_post_gain,
):
    tok_rows = queries.shape[0]
    tp_share = lax.axis_size("tp")
    part_rows = tok_rows // tp_share
    my_rows = lax.axis_index("tp") * part_rows
    side = lax.axis_index("grp")
    keys_values = lax.all_gather(jnp.concatenate([keys, values], axis=1), "sp", axis=0, tiled=True)
    gate_mine, gate_other = half_gather(gate_weight, side)
    up_mine, up_other = half_gather(up_weight, side)
    down_all = lax.all_gather(down_weight, "sp", axis=1, tiled=True)
    attended = stick_attention(queries, keys_values, lax.axis_index("sp") * tok_rows)
    mixed_sum = lax.psum(
        jnp.dot(attended, out_weight, preferred_element_type=jnp.float32).astype(jnp.bfloat16), "tp"
    ).astype(jnp.float32)
    first_all = residual.astype(jnp.float32) + rms_scale(mixed_sum, post_gain)
    ffn_in = rms_scale(first_all, ffn_pre_gain).astype(jnp.bfloat16)
    first_mine = lax.dynamic_slice_in_dim(first_all, my_rows, part_rows, 0)
    half = gate_weight.shape[0] // 2
    pieces = ffn_in.reshape(tok_rows, -1, 2, half)
    in_mine = lax.dynamic_index_in_dim(pieces, side, 2, False).reshape(tok_rows, -1)
    in_other = lax.dynamic_index_in_dim(pieces, 1 - side, 2, False).reshape(tok_rows, -1)
    gate_sum = jnp.dot(in_mine, gate_mine, preferred_element_type=jnp.float32) + jnp.dot(
        in_other, gate_other, preferred_element_type=jnp.float32
    )
    up_sum = jnp.dot(in_mine, up_mine, preferred_element_type=jnp.float32) + jnp.dot(
        in_other, up_other, preferred_element_type=jnp.float32
    )
    hidden = (jax.nn.silu(gate_sum) * up_sum).astype(jnp.bfloat16)
    ffn_terms = jnp.dot(
        hidden,
        down_all,
        preferred_element_type=jnp.float32,
    )
    ffn_out = lax.psum_scatter(
        ffn_terms.astype(jnp.bfloat16), "tp", scatter_dimension=0, tiled=True
    ).astype(jnp.float32)
    result = first_mine + 0.5 * rms_scale(ffn_out, ffn_post_gain)
    return result.astype(jnp.bfloat16)


def solution(mesh):
    in_specs = (
        P(("grp", "sp"), "tp"),
        P(("grp", "sp"), "tp"),
        P(("grp", "sp"), "tp"),
        P(("grp", "sp"), None),
        P("tp", None),
        P(),
        P("sp", "tp"),
        P("sp", "tp"),
        P("tp", "sp"),
        P(),
        P(),
    )
    out_specs = P(("grp", "sp", "tp"), None)
    return jax.shard_map(
        per_device, mesh=mesh, in_specs=in_specs, out_specs=out_specs, check_vma=False
    )
```

```python
import functools
import math

import jax
import jax.numpy as jnp
from jax import lax
from jax.experimental import pallas as pl
from jax.experimental.pallas import tpu as pltpu
from jax.sharding import PartitionSpec as P

HEAD_DIM = 64


norm_eps = 1e-06


def rms_scale(row_block, gain):
    mean_square = jnp.mean(row_block * row_block, axis=-1, keepdims=True)
    return row_block * lax.rsqrt(mean_square + norm_eps) * gain


def attention_block(q_ref, k_ref, v_ref, acc_ref, gone_ref, block_index, span, masked):
    rows = q_ref.shape[1]
    key_rows = pl.ds(pl.multiple_of(block_index * span, span), span)
    key_block = k_ref[key_rows, :]
    value_block = v_ref[key_rows, :]
    row_iota = lax.broadcasted_iota(jnp.int32, (span, span), 0)
    col_iota = lax.broadcasted_iota(jnp.int32, (span, span), 1)
    later = jnp.where(row_iota > col_iota, 1.0, 0.0).astype(jnp.bfloat16)
    lane_head = lax.broadcasted_iota(jnp.int32, acc_ref.shape, 1) // HEAD_DIM
    for head in range(q_ref.shape[0]):
        scores = lax.dot_general(
            q_ref[head], key_block, (((1,), (1,)), ((), ())), preferred_element_type=jnp.float32
        )
        soft = jnp.maximum(scores, 0.0) + jnp.log(1.0 + jnp.exp(-jnp.abs(scores)))
        expo = scores - soft
        if masked:
            strict = col_iota < row_iota
            soft = jnp.where(strict, soft, 0.0)
        tail = jnp.dot(soft.astype(jnp.bfloat16), later, preferred_element_type=jnp.float32)
        gone = gone_ref[head]
        wide = jnp.concatenate([gone] * (span // gone.shape[1]), axis=1)
        weights = jnp.exp(expo - (tail + wide))
        if masked:
            weights = jnp.where(strict, weights, 0.0)
        part = jnp.dot(
            weights.astype(jnp.bfloat16), value_block, preferred_element_type=jnp.float32
        )
        acc_ref[...] += jnp.where(lane_head == head, part, 0.0)
        total = tail[:, :1] + soft[:, :1]
        gone_ref[head] = gone + jnp.broadcast_to(total, gone.shape)


def attention_kernel(row_ref, q_ref, k_ref, v_ref, out_ref, acc_ref, gone_ref, *, span):
    diagonal = row_ref[0] // span + pl.program_id(1)
    acc_ref[...] = jnp.zeros_like(acc_ref)
    gone_ref[...] = jnp.zeros_like(gone_ref)
    attention_block(q_ref, k_ref, v_ref, acc_ref, gone_ref, diagonal, span, True)

    def turn(step, carry):
        attention_block(
            q_ref, k_ref, v_ref, acc_ref, gone_ref, diagonal - 1 - step, span, False
        )
        return carry

    lax.fori_loop(0, diagonal, turn, 0)
    out_ref[...] = acc_ref[...].astype(out_ref.dtype)


def stick_attention(queries, keys_values, first_row):
    tok_rows, width = queries.shape
    key_total = keys_values.shape[0]
    span = math.gcd(256, tok_rows)
    lanes = 128
    pack = lanes // HEAD_DIM
    column_groups = width // lanes
    lane_head = (jnp.arange(width) % lanes) // HEAD_DIM
    scaled = queries * jnp.asarray(1.0 / math.sqrt(HEAD_DIM), queries.dtype)
    split_queries = jnp.stack(
        [jnp.where(lane_head[None, :] == head, scaled, jnp.zeros_like(scaled)) for head in range(pack)]
    )
    grid_spec = pltpu.PrefetchScalarGridSpec(
        num_scalar_prefetch=1,
        grid=(column_groups, tok_rows // span),
        in_specs=[
            pl.BlockSpec((pack, span, lanes), lambda p, i, row: (0, i, p)),
            pl.BlockSpec((key_total, lanes), lambda p, i, row: (0, p)),
            pl.BlockSpec((key_total, lanes), lambda p, i, row: (0, column_groups + p)),
        ],
        out_specs=pl.BlockSpec((span, lanes), lambda p, i, row: (i, p)),
        scratch_shapes=[
            pltpu.VMEM((span, lanes), jnp.float32),
            pltpu.VMEM((pack, span, lanes), jnp.float32),
        ],
    )
    return pl.pallas_call(
        functools.partial(attention_kernel, span=span),
        grid_spec=grid_spec,
        out_shape=jax.ShapeDtypeStruct((tok_rows, width), jnp.bfloat16),
        compiler_params=pltpu.CompilerParams(vmem_limit_bytes=40 * 2**20),
        name="stick_attention",
    )(jnp.reshape(first_row, (1,)).astype(jnp.int32), split_queries, keys_values, keys_values)


def trade(block, k):
    count = lax.axis_size("tp")
    return lax.ppermute(block, "tp", [(i, i ^ k) for i in range(count)])


def half_gather(weight, side):
    half = weight.shape[0] // 2
    mine = lax.dynamic_slice_in_dim(weight, side * half, half, 0)
    mine = lax.all_gather(mine, "sp", axis=0, tiled=True)
    other = lax.ppermute(mine, "grp", [(0, 1), (1, 0)])
    return mine, other


def per_device(
    queries,
    keys,
    values,
    residual,
    out_weight,
    post_gain,
    gate_weight,
    up_weight,
    down_weight,
    ffn_pre_gain,
    ffn_post_gain,
):
    tok_rows = queries.shape[0]
    tp_share = lax.axis_size("tp")
    part_rows = tok_rows // tp_share
    my_rows = lax.axis_index("tp") * part_rows
    side = lax.axis_index("grp")
    keys_values = lax.all_gather(jnp.concatenate([keys, values], axis=1), "sp", axis=0, tiled=True)
    gate_mine, gate_other = half_gather(gate_weight, side)
    up_mine, up_other = half_gather(up_weight, side)
    down_all = lax.all_gather(down_weight, "sp", axis=1, tiled=True)
    attended = stick_attention(queries, keys_values, lax.axis_index("sp") * tok_rows)
    parts = jnp.dot(attended, out_weight, preferred_element_type=jnp.float32).astype(jnp.bfloat16)
    parts = parts.reshape(tp_share, part_rows, -1)
    me = lax.axis_index("tp")
    mixed_mine = lax.dynamic_index_in_dim(parts, me, 0, False).astype(jnp.float32)
    for k in range(1, tp_share):
        sent = lax.dynamic_index_in_dim(parts, jnp.bitwise_xor(me, k), 0, False)
        mixed_mine = mixed_mine + trade(sent, k).astype(jnp.float32)
    residual_mine = lax.dynamic_slice_in_dim(residual, my_rows, part_rows, 0)
    first_mine = residual_mine.astype(jnp.float32) + rms_scale(mixed_mine, post_gain)
    in_rows = rms_scale(first_mine, ffn_pre_gain).astype(jnp.bfloat16)
    ffn_in = jnp.concatenate(
        [in_rows] + [trade(in_rows, k) for k in range(1, tp_share)], axis=0
    )
    half = gate_weight.shape[0] // 2
    pieces = ffn_in.reshape(tok_rows, -1, 2, half)
    in_mine = lax.dynamic_index_in_dim(pieces, side, 2, False).reshape(tok_rows, -1)
    in_other = lax.dynamic_index_in_dim(pieces, 1 - side, 2, False).reshape(tok_rows, -1)
    gate_sum = jnp.dot(in_mine, gate_mine, preferred_element_type=jnp.float32) + jnp.dot(
        in_other, gate_other, preferred_element_type=jnp.float32
    )
    up_sum = jnp.dot(in_mine, up_mine, preferred_element_type=jnp.float32) + jnp.dot(
        in_other, up_other, preferred_element_type=jnp.float32
    )
    hidden = (jax.nn.silu(gate_sum) * up_sum).astype(jnp.bfloat16)
    near_rows = tok_rows // 2
    far_terms = jnp.dot(
        hidden[near_rows:], down_all, preferred_element_type=jnp.float32
    ).astype(jnp.bfloat16)
    near_terms = jnp.dot(
        hidden[:near_rows], down_all, preferred_element_type=jnp.float32
    ).astype(jnp.bfloat16)
    blocks = [
        near_terms[k * part_rows : (k + 1) * part_rows] for k in range(tp_share // 2)
    ] + [far_terms[k * part_rows : (k + 1) * part_rows] for k in range(tp_share // 2)]
    ffn_out = blocks[0].astype(jnp.float32)
    for k in range(tp_share - 1, 0, -1):
        ffn_out = ffn_out + trade(blocks[k], k).astype(jnp.float32)
    result = first_mine + 0.5 * rms_scale(ffn_out, ffn_post_gain)
    return result.astype(jnp.bfloat16)


def solution(mesh):
    in_specs = (
        P(("grp", "sp"), "tp"),
        P(("grp", "sp"), "tp"),
        P(("grp", "sp"), "tp"),
        P(("grp", "sp"), None),
        P("tp", None),
        P(),
        P("sp", "tp"),
        P("sp", "tp"),
        P("tp", "sp"),
        P(),
        P(),
    )
    out_specs = P(("grp", "sp", "tp"), None)
    return jax.shard_map(
        per_device, mesh=mesh, in_specs=in_specs, out_specs=out_specs, check_vma=False
    )
```

```python
import functools
import math

import jax
import jax.numpy as jnp
from jax import lax
from jax.experimental import pallas as pl
from jax.experimental.pallas import tpu as pltpu
from jax.sharding import PartitionSpec as P

HEAD_DIM = 64


norm_eps = 1e-06


def rms_scale(row_block, gain):
    mean_square = jnp.mean(row_block * row_block, axis=-1, keepdims=True)
    return row_block * lax.rsqrt(mean_square + norm_eps) * gain


def attention_block(q_ref, k_ref, v_ref, acc_ref, gone_ref, block_index, span, masked):
    rows = q_ref.shape[1]
    key_rows = pl.ds(pl.multiple_of(block_index * span, span), span)
    key_block = k_ref[key_rows, :]
    value_block = v_ref[key_rows, :]
    row_iota = lax.broadcasted_iota(jnp.int32, (span, span), 0)
    col_iota = lax.broadcasted_iota(jnp.int32, (span, span), 1)
    later = jnp.where(row_iota > col_iota, 1.0, 0.0).astype(jnp.bfloat16)
    lane_head = lax.broadcasted_iota(jnp.int32, acc_ref.shape, 1) // HEAD_DIM
    for head in range(q_ref.shape[0]):
        scores = lax.dot_general(
            q_ref[head], key_block, (((1,), (1,)), ((), ())), preferred_element_type=jnp.float32
        )
        soft = jnp.maximum(scores, 0.0) + jnp.log(1.0 + jnp.exp(-jnp.abs(scores)))
        expo = scores - soft
        if masked:
            strict = col_iota < row_iota
            soft = jnp.where(strict, soft, 0.0)
        tail = jnp.dot(soft.astype(jnp.bfloat16), later, preferred_element_type=jnp.float32)
        gone = gone_ref[head]
        wide = jnp.concatenate([gone] * (span // gone.shape[1]), axis=1)
        weights = jnp.exp(expo - (tail + wide))
        if masked:
            weights = jnp.where(strict, weights, 0.0)
        part = jnp.dot(
            weights.astype(jnp.bfloat16), value_block, preferred_element_type=jnp.float32
        )
        acc_ref[...] += jnp.where(lane_head == head, part, 0.0)
        total = tail[:, :1] + soft[:, :1]
        gone_ref[head] = gone + jnp.broadcast_to(total, gone.shape)


def attention_kernel(row_ref, q_ref, k_ref, v_ref, out_ref, acc_ref, gone_ref, *, span):
    diagonal = row_ref[0] // span + pl.program_id(1)
    acc_ref[...] = jnp.zeros_like(acc_ref)
    gone_ref[...] = jnp.zeros_like(gone_ref)
    attention_block(q_ref, k_ref, v_ref, acc_ref, gone_ref, diagonal, span, True)

    def turn(step, carry):
        attention_block(
            q_ref, k_ref, v_ref, acc_ref, gone_ref, diagonal - 1 - step, span, False
        )
        return carry

    lax.fori_loop(0, diagonal, turn, 0)
    out_ref[...] = acc_ref[...].astype(out_ref.dtype)


def stick_attention(queries, keys_values, first_row):
    tok_rows, width = queries.shape
    key_total = keys_values.shape[0]
    span = math.gcd(256, tok_rows)
    lanes = 128
    pack = lanes // HEAD_DIM
    column_groups = width // lanes
    lane_head = (jnp.arange(width) % lanes) // HEAD_DIM
    scaled = queries * jnp.asarray(1.0 / math.sqrt(HEAD_DIM), queries.dtype)
    split_queries = jnp.stack(
        [jnp.where(lane_head[None, :] == head, scaled, jnp.zeros_like(scaled)) for head in range(pack)]
    )
    grid_spec = pltpu.PrefetchScalarGridSpec(
        num_scalar_prefetch=1,
        grid=(column_groups, tok_rows // span),
        in_specs=[
            pl.BlockSpec((pack, span, lanes), lambda p, i, row: (0, i, p)),
            pl.BlockSpec((key_total, lanes), lambda p, i, row: (0, p)),
            pl.BlockSpec((key_total, lanes), lambda p, i, row: (0, column_groups + p)),
        ],
        out_specs=pl.BlockSpec((span, lanes), lambda p, i, row: (i, p)),
        scratch_shapes=[
            pltpu.VMEM((span, lanes), jnp.float32),
            pltpu.VMEM((pack, span, lanes), jnp.float32),
        ],
    )
    return pl.pallas_call(
        functools.partial(attention_kernel, span=span),
        grid_spec=grid_spec,
        out_shape=jax.ShapeDtypeStruct((tok_rows, width), jnp.bfloat16),
        compiler_params=pltpu.CompilerParams(vmem_limit_bytes=40 * 2**20),
        name="stick_attention",
    )(jnp.reshape(first_row, (1,)).astype(jnp.int32), split_queries, keys_values, keys_values)


def trade(block, k):
    count = lax.axis_size("tp")
    return lax.ppermute(block, "tp", [(i, i ^ k) for i in range(count)])


def half_gather(weight, side):
    half = weight.shape[0] // 2
    mine = lax.dynamic_slice_in_dim(weight, side * half, half, 0)
    mine = lax.all_gather(mine, "sp", axis=0, tiled=True)
    other = lax.ppermute(mine, "grp", [(0, 1), (1, 0)])
    return mine, other


def per_device(
    queries,
    keys,
    values,
    residual,
    out_weight,
    post_gain,
    gate_weight,
    up_weight,
    down_weight,
    ffn_pre_gain,
    ffn_post_gain,
):
    tok_rows = queries.shape[0]
    tp_share = lax.axis_size("tp")
    part_rows = tok_rows // tp_share
    my_rows = lax.axis_index("tp") * part_rows
    side = lax.axis_index("grp")
    keys_values = lax.all_gather(jnp.concatenate([keys, values], axis=1), "sp", axis=0, tiled=True)
    gate_mine, gate_other = half_gather(gate_weight, side)
    up_mine, up_other = half_gather(up_weight, side)
    swap_rows = down_weight.shape[0] // 5
    down_mine = lax.dynamic_slice_in_dim(down_weight, side * swap_rows, swap_rows, 0)
    down_mine = lax.all_gather(down_mine, "sp", axis=1, tiled=True)
    down_other = lax.ppermute(down_mine, "grp", [(0, 1), (1, 0)])
    down_top = jnp.concatenate(
        [
            jnp.where(side == 0, down_mine, down_other),
            jnp.where(side == 0, down_other, down_mine),
        ],
        axis=0,
    )
    top_rows = 2 * swap_rows
    down_rest = lax.all_gather(down_weight[top_rows:], "sp", axis=1, tiled=True)
    attended = stick_attention(queries, keys_values, lax.axis_index("sp") * tok_rows)
    parts = jnp.dot(attended, out_weight, preferred_element_type=jnp.float32).astype(jnp.bfloat16)
    parts = parts.reshape(tp_share, part_rows, -1)
    me = lax.axis_index("tp")
    mixed_mine = lax.dynamic_index_in_dim(parts, me, 0, False).astype(jnp.float32)
    for k in range(1, tp_share):
        sent = lax.dynamic_index_in_dim(parts, jnp.bitwise_xor(me, k), 0, False)
        mixed_mine = mixed_mine + trade(sent, k).astype(jnp.float32)
    residual_mine = lax.dynamic_slice_in_dim(residual, my_rows, part_rows, 0)
    first_mine = residual_mine.astype(jnp.float32) + rms_scale(mixed_mine, post_gain)
    in_rows = rms_scale(first_mine, ffn_pre_gain).astype(jnp.bfloat16)
    ffn_in = jnp.concatenate(
        [in_rows] + [trade(in_rows, k) for k in range(1, tp_share)], axis=0
    )
    half = gate_weight.shape[0] // 2
    pieces = ffn_in.reshape(tok_rows, -1, 2, half)
    in_mine = lax.dynamic_index_in_dim(pieces, side, 2, False).reshape(tok_rows, -1)
    in_other = lax.dynamic_index_in_dim(pieces, 1 - side, 2, False).reshape(tok_rows, -1)
    gate_sum = jnp.dot(in_mine, gate_mine, preferred_element_type=jnp.float32) + jnp.dot(
        in_other, gate_other, preferred_element_type=jnp.float32
    )
    up_sum = jnp.dot(in_mine, up_mine, preferred_element_type=jnp.float32) + jnp.dot(
        in_other, up_other, preferred_element_type=jnp.float32
    )
    hidden = (jax.nn.silu(gate_sum) * up_sum).astype(jnp.bfloat16)
    near_rows = tok_rows // 2
    far_terms = (
        jnp.dot(hidden[near_rows:, :top_rows], down_top, preferred_element_type=jnp.float32)
        + jnp.dot(hidden[near_rows:, top_rows:], down_rest, preferred_element_type=jnp.float32)
    ).astype(jnp.bfloat16)
    near_terms = (
        jnp.dot(hidden[:near_rows, :top_rows], down_top, preferred_element_type=jnp.float32)
        + jnp.dot(hidden[:near_rows, top_rows:], down_rest, preferred_element_type=jnp.float32)
    ).astype(jnp.bfloat16)
    blocks = [
        near_terms[k * part_rows : (k + 1) * part_rows] for k in range(tp_share // 2)
    ] + [far_terms[k * part_rows : (k + 1) * part_rows] for k in range(tp_share // 2)]
    ffn_out = blocks[0].astype(jnp.float32)
    for k in range(tp_share - 1, 0, -1):
        ffn_out = ffn_out + trade(blocks[k], k).astype(jnp.float32)
    result = first_mine + 0.5 * rms_scale(ffn_out, ffn_post_gain)
    return result.astype(jnp.bfloat16)


def solution(mesh):
    in_specs = (
        P(("grp", "sp"), "tp"),
        P(("grp", "sp"), "tp"),
        P(("grp", "sp"), "tp"),
        P(("grp", "sp"), None),
        P("tp", None),
        P(),
        P("sp", "tp"),
        P("sp", "tp"),
        P("tp", "sp"),
        P(),
        P(),
    )
    out_specs = P(("grp", "sp", "tp"), None)
    return jax.shard_map(
        per_device, mesh=mesh, in_specs=in_specs, out_specs=out_specs, check_vma=False
    )
```
